32 devices in a mesh: sp: 8 (over z, core), tp: 4 (over y, x).
Axes of the slice: x: 2, y: 2, z: 4, core: 2. Of those that a mesh axis runs over, the one named last changes fastest.
Arguments:
- u_val: bfloat16 [2048, 2048], P('sp', 'tp'), may hold values from -6 to 6
- u_gate: bfloat16 [2048, 2048], P('sp', 'tp'), may hold values from -9 to 9
- conv_weight: float32 [31, 2048], P(None, 'tp')
- conv_bias: float32 [2048], P('tp'), may hold values from -3 to 3
- ln_gain: float32 [2048], P('tp'), may hold values from 0.1 to 1.9
- ln_bias: float32 [2048], P('tp'), may hold values from -3 to 3
- proj_weight: bfloat16 [2048, 4096], P(None, 'tp'), may hold values from -0.125 to 0.125
- resid: bfloat16 [2048, 4096], P('sp', 'tp')
- norm_gain: float32 [4096], P('tp'), may hold values from 0.1 to 1.9
- route_ids: int32 [2048, 2], P('sp'), may hold values from 0 to 7, all different within a row; in each aligned block of 256 rows (0 to 255, 256 to 511, ...) at most 128 rows name the same one
- route_wts: float32 [2048, 2], P('sp'), may hold values from 0.3 to 1.5
- expert_gate: bfloat16 [8, 4096, 1024], P('sp', None, 'tp'), may hold values from -0.09375 to 0.09375
- expert_up: bfloat16 [8, 4096, 1024], P('sp', None, 'tp'), may hold values from -0.09375 to 0.09375
- expert_down: bfloat16 [8, 1024, 4096], P('sp', None, 'tp'), may hold values from -0.1875 to 0.1875
- shared_gate: bfloat16 [4096, 1024], P(None, 'tp'), may hold values from -0.09375 to 0.09375
- shared_up: bfloat16 [4096, 1024], P(None, 'tp'), may hold values from -0.09375 to 0.09375
- shared_down: bfloat16 [1024, 4096], P(None, 'tp'), may hold values from -0.1875 to 0.1875
Outputs:
- mixed: bfloat16 [2048, 4096], P('sp', 'tp')
The draws below stay inside these ranges and needn't reach their ends.
Inputs may be any that keep to these rules, and one draw needn't show every extreme that they name: `route_ids`: each row names 2 different experts. In each aligned block of 256 rows (the rows of one index of sp) no expert is named by more than 128 rows, a bound that some expert reaches in some blocks.
All inputs are finite; a program needn't handle non-finite values.
Results may differ from the reference program's by a relative error of at most 0.012.
Values may be sent and summed in bfloat16 or wider, within the bound.
A program may use at most 64 MiB of HBM per device.

```python
import math
import jax
import jax.numpy as jnp
import numpy as np
from jax import lax

D = 4096
CONV = 2048
EXPERT_HIDDEN = 1024
SHARED_HIDDEN = 1024
KERNEL = 31
TOP = 2
TOK_DEV = 256
TOKENS = 2048
EXPERTS = 8
CAP = 128
N_SP = 8


def draw_conv_weight(key, part):
    ramp = 4.0 ** (jnp.arange(CONV, dtype=jnp.float32) / (CONV - 1))
    base = jax.random.normal(key, (KERNEL, CONV), jnp.float32)
    return base * ramp[None, :] * KERNEL ** (-0.5)


def draw_resid(key, part):
    ramp = 3.0 ** (jnp.arange(D, dtype=jnp.float32) / (D - 1))
    base = jax.random.normal(key, (TOKENS, D), jnp.float32)
    return (base * ramp[None, :]).astype(jnp.bfloat16)


def levels(stream_key, shape, split, low, largest):
    def one(dim, blocks):
        steps = jax.random.uniform(jax.random.fold_in(jax.random.fold_in(stream_key, 6), dim), (blocks,), jnp.float32, low / len(split), largest / len(split))
        return jnp.repeat(jnp.exp(steps), shape[dim] // blocks).reshape((-1,) + (1,) * (len(shape) - dim - 1))

    gain = one(*split[0])
    for cut in split[1:]:
        gain = gain * one(*cut)
    return gain


def deal_out(own_key, own, number, rows, count, top, bound, lean):
    order = jax.random.permutation(own_key, count)
    crowded, common = shares(count, rows * top, bound, lean, True), shares(count, rows * top, bound, lean, False)
    places = jnp.arange(count)

    def named(tallies, offset_by):
        used = int((tallies > 0).sum())
        fixed = max(1, used // 4)
        moved = fixed + (places - fixed + offset_by * (used - fixed)) % max(1, count - fixed)
        return jnp.zeros((count,), jnp.int32).at[order[jnp.where(places < fixed, places, moved)]].set(jnp.asarray(tallies, jnp.int32))

    tallies = jnp.where(number % 4 == 0, named(crowded, number // 4), named(common, number - number // 4 - 1))
    mixed = jax.random.permutation(jax.random.fold_in(own, 3), count)
    source_of, taker = mixed[0:count // 2 * 2:2], mixed[1:count // 2 * 2:2]
    room = jnp.minimum(tallies[source_of] - 1, bound - tallies[taker]) // 2
    room = jnp.where((source_of == order[0]) | (taker == order[0]) | (tallies[taker] == 0), 0, jnp.maximum(room, 0))
    moved = jax.random.randint(jax.random.fold_in(own, 4), (count // 2,), 0, 1 << 20) % (room + 1)
    tallies = tallies.at[source_of].add(-moved).at[taker].add(moved)
    members = jnp.searchsorted(jnp.cumsum(tallies), jnp.arange(rows * top), side="right").astype(jnp.int32)
    listing = members.reshape(top, rows).T
    listing = listing[jax.random.permutation(jax.random.fold_in(own, 1), rows)]
    offset_by = jax.random.randint(jax.random.fold_in(own, 2), (rows, 1), 0, top)
    return jnp.take_along_axis(listing, (jnp.arange(top)[None, :] + offset_by) % top, axis=1)


def shares(amount, total, reach, lean, full):
    portions = [(1 << 20) // math.isqrt(standing ** lean) + 1 for standing in range(1, amount + 1)]
    largest = reach if full else min(reach, max(-(-total // amount), total * portions[0] // sum(portions)))
    least = 1 if total - largest >= amount - 1 else 0
    holding, rest = [largest] + [least] * (amount - 1), total - largest - least * (amount - 1)
    while rest > 0:
        free = [i for i in range(1, amount) if holding[i] < largest] or [i for i in range(1, amount) if holding[i] < reach]
        whole, left = sum([portions[i] for i in free]), rest
        for i in free:
            more = min(reach - holding[i], max(1, left * portions[i] // whole), rest)
            holding[i] = holding[i] + more
            rest = rest - more
    return np.array(holding)


def normal_values(stream_key, shape, scale, reach, split=(), kind=jnp.bfloat16):
    drawn = jax.random.normal(stream_key, shape, jnp.float32) * scale
    if len(split) > 0:
        drawn = levels(stream_key, shape, split, -0.22, 0.18) * drawn
    return jnp.clip(drawn, min=-reach, max=reach).astype(kind)


def setup_inputs(seed: int = 0) -> dict:
    arg_keys = jax.random.split(jax.random.key(seed), 18)
    u_val = normal_values(arg_keys[0], (TOKENS, CONV), 1.0, 6.0, ((0, 8), (1, 4)))
    u_gate = normal_values(arg_keys[1], (TOKENS, CONV), 1.5, 9.0, ((0, 8), (1, 4)))
    conv_weight = draw_conv_weight(jax.random.fold_in(arg_keys[17], 71), 0)
    conv_bias = normal_values(arg_keys[3], (CONV,), 0.5, 3.0, ((0, 4),), jnp.float32)
    ln_gain = jnp.clip(1.0 + 0.18 * jax.random.normal(arg_keys[4], (CONV,), jnp.float32), 0.1, 1.9)
    ln_bias = normal_values(arg_keys[5], (CONV,), 0.5, 3.0, ((0, 4),), jnp.float32)
    proj_weight = normal_values(arg_keys[6], (CONV, D), CONV ** -0.5, 0.125, ((1, 4),))
    resid = draw_resid(jax.random.fold_in(arg_keys[17], 71), 0)
    norm_gain = jnp.clip(1.0 + 0.18 * jax.random.normal(arg_keys[8], (D,), jnp.float32), 0.1, 1.9)
    route_ids_keys = jax.random.split(jax.random.fold_in(arg_keys[9], 1), TOKENS // TOK_DEV)
    route_ids_turns = jax.random.permutation(jax.random.fold_in(arg_keys[9], 3), TOKENS // TOK_DEV)
    route_ids = jax.vmap(lambda own, number: deal_out(jax.random.fold_in(arg_keys[9], 2), own, number, TOK_DEV, EXPERTS, TOP, CAP, 2))(route_ids_keys, route_ids_turns).reshape((TOKENS, TOP))
    route_wts = jnp.clip(0.3 + 1.2 * jax.random.uniform(arg_keys[10], (TOKENS, TOP), jnp.float32) ** levels(arg_keys[10], (TOKENS, TOP), ((0, 8),), -0.2, 0.2), 0.3, 1.5)
    expert_gate = normal_values(arg_keys[11], (EXPERTS, D, EXPERT_HIDDEN), D ** -0.5, 0.09375, ((0, 8), (2, 4)))
    expert_up = normal_values(arg_keys[12], (EXPERTS, D, EXPERT_HIDDEN), D ** -0.5, 0.09375, ((0, 8), (2, 4)))
    expert_down = normal_values(arg_keys[13], (EXPERTS, EXPERT_HIDDEN, D), EXPERT_HIDDEN ** -0.5, 0.1875, ((0, 8), (2, 4)))
    shared_gate = normal_values(arg_keys[14], (D, SHARED_HIDDEN), D ** -0.5, 0.09375, ((1, 4),))
    shared_up = normal_values(arg_keys[15], (D, SHARED_HIDDEN), D ** -0.5, 0.09375, ((1, 4),))
    shared_down = normal_values(arg_keys[16], (SHARED_HIDDEN, D), SHARED_HIDDEN ** -0.5, 0.1875, ((1, 4),))
    return {"u_val": u_val, "u_gate": u_gate, "conv_weight": conv_weight, "conv_bias": conv_bias, "ln_gain": ln_gain, "ln_bias": ln_bias, "proj_weight": proj_weight, "resid": resid, "norm_gain": norm_gain, "route_ids": route_ids, "route_wts": route_wts, "expert_gate": expert_gate, "expert_up": expert_up, "expert_down": expert_down, "shared_gate": shared_gate, "shared_up": shared_up, "shared_down": shared_down}


norm_eps = 1e-06

def slot_table(block_ids, block_wts):
    pair_ids = block_ids.reshape(-1)
    pair_wts = block_wts.reshape(-1)
    onehot = (pair_ids[:, None] == jnp.arange(EXPERTS, dtype=jnp.int32)[None, :]).astype(jnp.int32)
    before = jnp.cumsum(onehot, axis=0) - onehot
    position = lax.optimization_barrier(jnp.sum(before * onehot, axis=1))
    pair_slot = pair_ids * CAP + position
    matches = (jnp.arange(EXPERTS * CAP, dtype=jnp.int32)[:, None] == pair_slot[None, :]).astype(jnp.int32)
    pair_tok = (jnp.arange(TOK_DEV * TOP, dtype=jnp.int32) // TOP).astype(jnp.int32)
    filled = lax.optimization_barrier(jnp.sum(matches, axis=1))
    slot_tok = lax.optimization_barrier(jnp.sum(matches * pair_tok[None, :], axis=1)) + (1 - filled) * TOK_DEV
    slot_wts = lax.optimization_barrier(jnp.sum(matches.astype(jnp.float32) * pair_wts[None, :], axis=1))
    return (slot_tok.astype(jnp.int32), slot_wts)

def reference(u_val, u_gate, conv_weight, conv_bias, ln_gain, ln_bias, proj_weight, resid, norm_gain, route_ids, route_wts, expert_gate, expert_up, expert_down, shared_gate, shared_up, shared_down):
    gated = (u_val.astype(jnp.float32) * jax.nn.sigmoid(u_gate.astype(jnp.float32))).astype(jnp.bfloat16)
    gated = lax.optimization_barrier(gated).astype(jnp.float32)
    padded = jnp.concatenate([jnp.zeros((KERNEL - 1, CONV), jnp.float32), gated], axis=0)
    conv_sum = jnp.zeros((TOKENS, CONV), jnp.float32) + conv_bias[None, :]
    for tap_index in range(KERNEL):
        conv_sum = conv_sum + conv_weight[tap_index][None, :] * padded[tap_index:tap_index + TOKENS]
    channel_mean = lax.optimization_barrier(jnp.mean(conv_sum, axis=1, keepdims=True))
    centered = conv_sum - channel_mean
    channel_var = lax.optimization_barrier(jnp.mean(centered * centered, axis=1, keepdims=True))
    conv_out = jax.nn.silu(centered * lax.rsqrt(channel_var + norm_eps) * ln_gain + ln_bias).astype(jnp.bfloat16)
    projected = jnp.dot(conv_out, proj_weight, preferred_element_type=jnp.float32)
    residual_mid = (resid.astype(jnp.float32) + projected).astype(jnp.bfloat16)
    residual_wide = residual_mid.astype(jnp.float32)
    mean_square = lax.optimization_barrier(jnp.mean(residual_wide * residual_wide, axis=1, keepdims=True))
    normed_rows = (residual_wide * lax.rsqrt(mean_square + norm_eps) * norm_gain).astype(jnp.bfloat16)
    shared_hidden = (jax.nn.silu(jnp.dot(normed_rows, shared_gate, preferred_element_type=jnp.float32)) * jnp.dot(normed_rows, shared_up, preferred_element_type=jnp.float32)).astype(jnp.bfloat16)
    shared_out = jnp.dot(shared_hidden, shared_down, preferred_element_type=jnp.float32)
    slot_tok, slot_wts = jax.vmap(slot_table)(route_ids.reshape(N_SP, TOK_DEV, TOP), route_wts.reshape(N_SP, TOK_DEV, TOP))
    offsets = (jnp.arange(N_SP, dtype=jnp.int32) * TOK_DEV)[:, None]
    global_tok = jnp.where(slot_tok < TOK_DEV, slot_tok + offsets, TOKENS).astype(jnp.int32)
    global_tok = global_tok.reshape(N_SP, EXPERTS, CAP).transpose(1, 0, 2).reshape(EXPERTS, N_SP * CAP)
    slot_wts = slot_wts.reshape(N_SP, EXPERTS, CAP).transpose(1, 0, 2).reshape(EXPERTS, N_SP * CAP)
    rows_ext = jnp.concatenate([normed_rows, jnp.zeros((1, D), jnp.bfloat16)], axis=0)

    def expert_step(total, inputs):
        gate_w, up_w, down_w, tok_ids, tok_wts = inputs
        slot_rows = jnp.take(rows_ext, tok_ids, axis=0)
        hidden = (jax.nn.silu(jnp.dot(slot_rows, gate_w, preferred_element_type=jnp.float32)) * jnp.dot(slot_rows, up_w, preferred_element_type=jnp.float32)).astype(jnp.bfloat16)
        expert_out = jnp.dot(hidden, down_w, preferred_element_type=jnp.float32).astype(jnp.bfloat16)
        weighted = expert_out.astype(jnp.float32) * tok_wts[:, None]
        return (total + jax.ops.segment_sum(weighted, tok_ids, num_segments=TOKENS + 1), None)
    routed, _ = lax.scan(expert_step, jnp.zeros((TOKENS + 1, D), jnp.float32), (expert_gate, expert_up, expert_down, global_tok, slot_wts))
    return (residual_wide + shared_out + routed[:TOKENS]).astype(jnp.bfloat16)
```

```python
import functools

import jax
import jax.numpy as jnp
from jax import lax
from jax.experimental import pallas as pl
from jax.experimental.pallas import tpu as pltpu
from jax.sharding import PartitionSpec as P

D = 4096
CONV = 2048


norm_eps = 1e-06


def shifted(block, axis, distance):
    devices = range(lax.axis_size(axis))
    route = [(i - distance, i) for i in devices if i - distance in devices]
    return lax.ppermute(block, axis, route)


def shards(
    u_val,
    u_gate,
    conv_weight,
    conv_bias,
    ln_gain,
    ln_bias,
    proj_weight,
    resid,
    norm_gain,
    route_ids,
    route_wts,
    expert_gate,
    expert_up,
    expert_down,
    shared_gate,
    shared_up,
    shared_down,
):
    tok_rows = u_val.shape[0]
    sp_count = lax.axis_size("sp")
    tp_count = lax.axis_size("tp")
    kernel_width = conv_weight.shape[0]
    gated = (u_val.astype(jnp.float32) * jax.nn.sigmoid(u_gate.astype(jnp.float32))).astype(
        jnp.bfloat16
    )
    rim_rows = shifted(gated[tok_rows - (kernel_width - 1) :], "sp", 1)
    padded = lax.optimization_barrier(jnp.concatenate([rim_rows, gated], axis=0)).astype(
        jnp.float32
    )
    conv_sum = jnp.zeros((tok_rows, gated.shape[1]), jnp.float32) + conv_bias[None, :]
    for tap_index in range(kernel_width):
        conv_sum = (
            conv_sum + conv_weight[tap_index][None, :] * padded[tap_index : tap_index + tok_rows]
        )
    stat_sums = lax.psum((jnp.sum(conv_sum, axis=1), jnp.sum(conv_sum * conv_sum, axis=1)), "tp")
    channel_mean = stat_sums[0] / CONV
    channel_var = stat_sums[1] / CONV - channel_mean * channel_mean
    normed_conv = (conv_sum - channel_mean[:, None]) * lax.rsqrt(channel_var + norm_eps)[:, None]
    conv_out = jax.nn.silu(normed_conv * ln_gain + ln_bias).astype(jnp.bfloat16)
    projected = jnp.dot(
        lax.all_gather(conv_out, "tp", axis=1, tiled=True),
        proj_weight,
        preferred_element_type=jnp.float32,
    )
    residual_mid = (resid.astype(jnp.float32) + projected).astype(jnp.bfloat16)
    residual_wide = residual_mid.astype(jnp.float32)
    square_sum = lax.psum(jnp.sum(residual_wide * residual_wide, axis=1), "tp")
    normed_rows = (
        residual_wide * lax.rsqrt(square_sum / D + norm_eps)[:, None] * norm_gain
    ).astype(jnp.bfloat16)
    rows_full = lax.all_gather(normed_rows, "tp", axis=1, tiled=True)
    topk_count = route_ids.shape[1]
    capacity = 2 * tok_rows * topk_count // sp_count
    pair_ids = route_ids.reshape(-1)
    onehot = (pair_ids[:, None] == jnp.arange(sp_count, dtype=jnp.int32)[None, :]).astype(jnp.int32)
    before = jnp.cumsum(onehot, axis=0) - onehot
    position = jnp.sum(before * onehot, axis=1)
    pair_slot = pair_ids * capacity + position
    matches = (
        jnp.arange(sp_count * capacity, dtype=jnp.int32)[:, None] == pair_slot[None, :]
    ).astype(jnp.int32)
    pair_tok = jnp.arange(tok_rows * topk_count, dtype=jnp.int32) // topk_count
    filled = jnp.sum(matches, axis=1)
    slot_tok = jnp.sum(matches * pair_tok[None, :], axis=1) + (1 - filled) * tok_rows
    rows_ext = jnp.concatenate(
        [rows_full, jnp.zeros((1, rows_full.shape[1]), jnp.bfloat16)], axis=0
    )
    part_slots = capacity // tp_count
    tp_index = lax.axis_index("tp")
    local_slots = lax.dynamic_slice_in_dim(
        slot_tok.reshape(sp_count, capacity), tp_index * part_slots, part_slots, 1
    )
    send_rows = jnp.take(rows_ext, local_slots.reshape(-1), axis=0).reshape(
        sp_count, part_slots, -1
    )
    received = lax.all_to_all(send_rows, "sp", split_axis=0, concat_axis=0, tiled=True)
    arrived = lax.all_gather(received, "tp", axis=1, tiled=True)
    slot_rows = arrived.reshape(sp_count * capacity, -1)
    gate_pre = jnp.dot(slot_rows, expert_gate[0], preferred_element_type=jnp.float32)
    up_proj = jnp.dot(slot_rows, expert_up[0], preferred_element_type=jnp.float32)
    hidden = (jax.nn.silu(gate_pre) * up_proj).astype(jnp.bfloat16)
    shared_pre = jnp.dot(rows_full, shared_gate, preferred_element_type=jnp.float32)
    shared_upper = jnp.dot(rows_full, shared_up, preferred_element_type=jnp.float32)
    shared_hidden = (jax.nn.silu(shared_pre) * shared_upper).astype(jnp.bfloat16)
    out_cols = expert_down.shape[2]
    routed_rows = expert_down[0]
    routed_out = jnp.dot(
        lax.all_gather(hidden, "tp", axis=1, tiled=True),
        routed_rows,
        preferred_element_type=jnp.float32,
    )
    shared_out = jnp.dot(
        lax.all_gather(shared_hidden, "tp", axis=1, tiled=True),
        shared_down,
        preferred_element_type=jnp.float32,
    )
    expert_rows = routed_out.astype(jnp.bfloat16).reshape(sp_count, capacity, out_cols)
    returned_rows = lax.all_to_all(expert_rows, "sp", split_axis=0, concat_axis=0, tiled=True)
    returned_flat = returned_rows.reshape(sp_count * capacity, out_cols)
    picked = (
        jnp.take(returned_flat, pair_slot, axis=0)
        .astype(jnp.float32)
        .reshape(tok_rows, topk_count, out_cols)
    )
    routed = jnp.sum(picked * route_wts[:, :, None], axis=1)
    return (residual_wide + shared_out + routed).astype(jnp.bfloat16)


VMEM = pltpu.VMEM
DMA = pltpu.SemaphoreType.DMA
F32 = jnp.float32
BF16 = jnp.bfloat16


def rcopy(src, dst, send_sem, recv_sem, device):
    return pltpu.make_async_remote_copy(
        src_ref=src,
        dst_ref=dst,
        send_sem=send_sem,
        recv_sem=recv_sem,
        device_id=device,
        device_id_type=pl.DeviceIdType.MESH,
    )


def dot(a, b):
    return jnp.dot(a, b, preferred_element_type=F32)


def greet(nsp, ntp, me, t):
    barrier = pltpu.get_barrier_semaphore()
    for j in range(1, ntp):
        pl.semaphore_signal(
            barrier, inc=1, device_id=(me, (t + j) % ntp), device_id_type=pl.DeviceIdType.MESH
        )
    for j in range(1, nsp):
        pl.semaphore_signal(
            barrier, inc=1, device_id=((me + j) % nsp, t), device_id_type=pl.DeviceIdType.MESH
        )
    pl.semaphore_wait(barrier, ntp - 1 + nsp - 1)


def front_kernel(
    nsp, ntp,
    conv, gain, bias, resid, ngain, route, proj_hbm,
    normed, mid, route_all,
    proj, gbuf, st, st2, rbuf,
    lsem, gsend, grecv, ssend, srecv, s2send, s2recv, rsend, rrecv,
):
    me = lax.axis_index("sp")
    t = lax.axis_index("tp")
    tok = conv.shape[0]
    weights = pltpu.make_async_copy(proj_hbm, proj, lsem.at[0])
    weights.start()
    greet(nsp, ntp, me, t)
    tables = []
    for j in range(1, nsp):
        e = (me + j) % nsp
        copy = rcopy(route.at[e], rbuf.at[me], rsend.at[j - 1], rrecv.at[j - 1], (e, t))
        copy.start()
        tables.append(copy)
    rbuf[me] = route[me]

    def exchange(stat, columns, send, recv):
        lane = lax.broadcasted_iota(jnp.int32, (tok, 128), 1)
        packed = jnp.zeros((tok, 128), F32)
        for i, column in enumerate(columns):
            packed = packed + jnp.where(lane == i, column, 0.0)
        stat[t] = jnp.transpose(packed)[0:8, :]
        copies = []
        for j in range(1, ntp):
            copy = rcopy(
                stat.at[t], stat.at[t], send.at[j - 1], recv.at[j - 1], (me, (t + j) % ntp)
            )
            copy.start()
            copies.append(copy)
        for copy in copies:
            copy.wait()
        total = stat[0]
        for i in range(1, ntp):
            total = total + stat[i]
        return jnp.transpose(jnp.concatenate([total] * 16, axis=0))

    x = conv[...]
    sums = exchange(
        st,
        [jnp.sum(x, axis=1, keepdims=True), jnp.sum(x * x, axis=1, keepdims=True)],
        ssend,
        srecv,
    )
    channels = conv.shape[1] * ntp
    mean = sums[:, 0:1] / channels
    var = sums[:, 1:2] / channels - mean * mean
    v = (x - mean) * lax.rsqrt(var + norm_eps) * gain[...] + bias[...]
    gbuf[t] = (v / (1.0 + jnp.exp(-v))).astype(BF16)
    copies = []
    for j in range(1, ntp):
        copy = rcopy(gbuf.at[t], gbuf.at[t], gsend.at[j - 1], grecv.at[j - 1], (me, (t + j) % ntp))
        copy.start()
        copies.append(copy)
    weights.wait()
    total = resid[...].astype(F32) + dot(gbuf[t], proj[t])
    for j in range(1, ntp):
        copies[j - 1].wait_recv()
        q = (t - j + ntp) % ntp
        total = total + dot(gbuf[q], proj[q])
    mid[...] = total.astype(BF16)
    wide = mid[...].astype(F32)
    squares = exchange(st2, [jnp.sum(wide * wide, axis=1, keepdims=True)], s2send, s2recv)
    scale = lax.rsqrt(squares[:, 0:1] / (mid.shape[1] * ntp) + norm_eps)
    normed[...] = (wide * scale * ngain[...]).astype(BF16)
    for copy in copies:
        copy.wait_send()
    for copy in tables:
        copy.wait()
    route_all[...] = rbuf[...]


def expert_kernel(
    nsp, ntp, cap,
    normed, mid, route, poscol, wg_h, wu_h, sg_h, su_h, wd_h, sd_h,
    out,
    buf, wg, wu, sg, su, wd, sd, acc, hid, shid, osend, ret,
    lsem, recv, zsend, xsend, ysend, relay, dsend, hsend, hrecv, shsend, shrecv, osem, orecv,
):
    me = lax.axis_index("sp")
    t = lax.axis_index("tp")
    tok, width = normed.shape
    half = tok // 2
    hidden_width = wg.shape[2]
    nz = nsp // 2
    z = me // 2
    c = me % 2
    partner = me + 1 - 2 * c
    t1 = t + 1 - 2 * (t % 2)
    t2 = t + 2 - 4 * (t // 2)
    t3 = 3 - t
    loads = [
        pltpu.make_async_copy(a, b, lsem.at[i])
        for i, (a, b) in enumerate(
            [(wg_h, wg), (wu_h, wu), (sg_h, sg), (su_h, su), (wd_h, wd), (sd_h, sd)]
        )
    ]
    own = pltpu.make_async_copy(normed, buf.at[me, t], lsem.at[6])
    own.start()
    for load in loads:
        load.start()
    greet(nsp, ntp, me, t)
    own.wait()

    def rows(b, q, h):
        return buf.at[b, q, pl.ds(h * half, half)]

    def push(b, q, h, sem, device):
        return rcopy(rows(b, q, h), rows(b, q, h), sem, recv.at[b, q, h], device)

    def arrived(b, q, h):
        push(b, q, h, zsend.at[0, 0], (me, t1)).wait_recv()

    def spread(k, b):
        copies = []
        for h in range(2):
            copies.append(push(b, t, h, xsend.at[k, h], (me, t1)))
            copies.append(push(b, t, h, ysend.at[k, h], (me, t2)))
            copies.append(push(b, t, h, dsend.at[k, 0, h], (partner, t)))
        return copies

    def relays(k, b):
        return [
            push(b, t1, 0, relay.at[k, 0], (me, t2)),
            push(b, t2, 1, relay.at[k, 1], (me, t1)),
        ]

    def across(k, b, i, q, h):
        return push(b, q, h, dsend.at[k, i, h], (partner, t))

    far = []
    for k in range(1, nz):
        for h in range(2):
            far.append(push(me, t, h, zsend.at[k - 1, h], (2 * ((z + k) % nz) + c, t)))
    for copy in far:
        copy.start()
    for copy in spread(0, me):
        copy.start()
    for load in loads:
        load.wait()

    def gate_up(i, b, q, first):
        data = buf[b, q]
        g = dot(data, wg[q])
        u = dot(data, wu[q])
        if first:
            acc[i, 0] = g
            acc[i, 1] = u
        else:
            acc[i, 0] += g
            acc[i, 1] += u

    def selection(b):
        slot = lax.broadcasted_iota(jnp.int32, (cap, tok), 0).astype(F32)
        return jnp.where(slot == route[b, 0:1, :], 1.0, 0.0)

    def hidden_copies(b):
        return [
            rcopy(hid.at[b, t], hid.at[b, t], hsend.at[b, j - 1], hrecv.at[b, j - 1],
                  (me, (t + j) % ntp))
            for j in range(1, ntp)
        ]

    def shared_copies():
        return [
            rcopy(shid.at[t], shid.at[t], shsend.at[j - 1], shrecv.at[j - 1], (me, (t + j) % ntp))
            for j in range(1, ntp)
        ]

    def gated(g, u):
        return (g / (1.0 + jnp.exp(-g)) * u).astype(BF16)

    def finish(i, b):
        hs = dot(selection(b).astype(BF16), gated(acc[i, 0], acc[i, 1]))
        hid[b, t] = hs.astype(BF16)
        for copy in hidden_copies(b):
            copy.start()

    def home(b):
        return rcopy(osend.at[b], ret.at[me], osem.at[b], orecv.at[me], (b, t))

    def down(b):
        for j in range(1, ntp):
            q = (t - j + ntp) % ntp
            rcopy(hid.at[b, q], hid.at[b, q], hsend.at[b, j - 1], hrecv.at[b, j - 1],
                  (me, t1)).wait_recv()
        o = dot(hid[b, 0], wd[0])
        for q in range(1, ntp):
            o = o + dot(hid[b, q], wd[q])
        weight = jnp.sum(selection(b) * route[b, 1:2, :], axis=1, keepdims=True)
        return (o * weight).astype(BF16)

    def step(k, carry):
        zk = (z - k + nz) % nz

        @pl.when(k < nz)
        def _():
            b = 2 * zk + c
            pb = 2 * zk + 1 - c
            forward = relays(k, b)
            for h in range(2):
                arrived(b, t1, h)
                if h == 0:
                    forward[0].start()
                across(k, b, 1, t1, h).start()
            for h in range(2):
                arrived(b, t2, h)
                if h == 1:
                    forward[1].start()
                across(k, b, 2, t2, h).start()

            @pl.when(k < nz - 1)
            def _():
                bn = 2 * ((z - k - 1 + nz) % nz) + c
                for h in range(2):
                    arrived(bn, t, h)
                for copy in spread(k + 1, bn):
                    copy.start()

            gate_up(0, b, t, True)
            gate_up(0, b, t1, False)
            gate_up(0, b, t2, False)
            for i, q in enumerate((t, t1, t2)):
                for h in range(2):
                    arrived(pb, q, h)
                gate_up(1, pb, q, i == 0)
            for h in range(2):
                arrived(b, t3, h)
                across(k, b, 3, t3, h).start()
            gate_up(0, b, t3, False)
            finish(0, b)
            for h in range(2):
                arrived(pb, t3, h)
            gate_up(1, pb, t3, False)
            finish(1, pb)

        @pl.when(k == 0)
        def _():
            def quarter(q, state):
                data = buf[me, q]
                g = dot(data, sg[q])
                u = dot(data, su[q])
                acc[0, 0] = jnp.where(q == 0, g, acc[0, 0] + g)
                acc[0, 1] = jnp.where(q == 0, u, acc[0, 1] + u)
                return state

            lax.fori_loop(0, ntp, quarter, 0)
            shid[t] = gated(acc[0, 0], acc[0, 1])
            for copy in shared_copies():
                copy.start()

        @pl.when(k == 1)
        def _():
            ret[me] = down(me)
            osend[partner] = down(partner)
            home(partner).start()

        @pl.when(k > 1)
        def _():
            zp = (z - k + 1 + nz) % nz

            def one(i, state):
                b = 2 * zp + i
                osend[b] = down(b)
                home(b).start()
                return state

            lax.fori_loop(0, 2, one, 0)

        return carry

    lax.fori_loop(0, nz + 1, step, 0)

    for copy in shared_copies():
        copy.wait_send()
    for j in range(1, ntp):
        q = (t - j + ntp) % ntp
        rcopy(shid.at[q], shid.at[q], shsend.at[j - 1], shrecv.at[j - 1], (me, t1)).wait_recv()
    total = mid[...].astype(F32)
    for q in range(ntp):
        total = total + dot(shid[q], sd[q])

    def drain(k, carry):
        b = 2 * ((z - k + nz) % nz) + c
        for copy in spread(k, b) + relays(k, b):
            copy.wait_send()
        for i, q in ((1, t1), (2, t2), (3, t3)):
            for h in range(2):
                across(k, b, i, q, h).wait_send()
        return carry

    lax.fori_loop(0, nz, drain, 0)
    for copy in far:
        copy.wait_send()

    def drain_hidden(b, carry):
        for copy in hidden_copies(b):
            copy.wait_send()
        return carry

    lax.fori_loop(0, nsp, drain_hidden, 0)
    for j in range(1, nsp):
        e = (me + j) % nsp
        rcopy(osend.at[e], ret.at[e], osem.at[e], orecv.at[e], (e, t)).wait()
    lane = lax.broadcasted_iota(jnp.int32, (tok, cap), 1).astype(F32)
    for e in range(nsp):
        pick = jnp.where(lane == poscol[:, e : e + 1], 1.0, 0.0).astype(BF16)
        total = total + dot(pick, ret[e])
    out[...] = total.astype(BF16)


def fast_shards(
    u_val, u_gate, conv_weight, conv_bias, ln_gain, ln_bias, proj_weight, resid, norm_gain,
    route_ids, route_wts, expert_gate, expert_up, expert_down, shared_gate, shared_up, shared_down,
):
    tok = u_val.shape[0]
    nsp = lax.axis_size("sp")
    ntp = lax.axis_size("tp")
    taps = conv_weight.shape[0]
    gated = (u_val.astype(F32) * jax.nn.sigmoid(u_gate.astype(F32))).astype(BF16)
    rim = shifted(gated[tok - (taps - 1) :], "sp", 1)
    padded = lax.optimization_barrier(jnp.concatenate([rim, gated], axis=0)).astype(F32)
    conv_sum = jnp.zeros((tok, gated.shape[1]), F32) + conv_bias[None, :]
    for i in range(taps):
        conv_sum = conv_sum + conv_weight[i][None, :] * padded[i : i + tok]

    top = route_ids.shape[1]
    cap = 2 * tok * top // nsp
    experts = jnp.arange(nsp, dtype=jnp.int32)
    named = jnp.zeros((nsp, tok), F32)
    weight = jnp.zeros((nsp, tok), F32)
    for k in range(top):
        hit = route_ids[:, k][None, :] == experts[:, None]
        named = named + hit.astype(F32)
        weight = weight + jnp.where(hit, route_wts[:, k][None, :], 0.0)
    earlier = (jnp.arange(tok)[:, None] < jnp.arange(tok)[None, :]).astype(BF16)
    pos = jnp.where(named > 0, dot(named.astype(BF16), earlier), -1.0)
    table = jnp.concatenate(
        [pos[:, None, :], weight[:, None, :], jnp.zeros((nsp, 6, tok), F32)], axis=1
    )
    poscol = jnp.concatenate([pos.T, jnp.full((tok, 128 - nsp), -1.0, F32)], axis=1)

    ch = conv_sum.shape[1]
    width = resid.shape[1]
    vm = pl.BlockSpec(memory_space=VMEM)
    hbm = pl.BlockSpec(memory_space=pl.ANY)
    normed, mid, route_all = pl.pallas_call(
        functools.partial(front_kernel, nsp, ntp),
        out_shape=[
            jax.ShapeDtypeStruct((tok, width), BF16),
            jax.ShapeDtypeStruct((tok, width), BF16),
            jax.ShapeDtypeStruct((nsp, 8, tok), F32),
        ],
        in_specs=[vm] * 6 + [hbm],
        out_specs=[vm] * 3,
        scratch_shapes=[
            VMEM((ntp, ch, width), BF16),
            VMEM((ntp, tok, ch), BF16),
            VMEM((ntp, 8, tok), F32),
            VMEM((ntp, 8, tok), F32),
            VMEM((nsp, 8, tok), F32),
            DMA((1,)),
            DMA((ntp - 1,)), DMA((ntp - 1,)),
            DMA((ntp - 1,)), DMA((ntp - 1,)),
            DMA((ntp - 1,)), DMA((ntp - 1,)),
            DMA((nsp - 1,)), DMA((nsp - 1,)),
        ],
        compiler_params=pltpu.CompilerParams(
            collective_id=1, has_side_effects=True, vmem_limit_bytes=24 << 20
        ),
        name="front",
    )(
        conv_sum, ln_gain[None, :], ln_bias[None, :], resid, norm_gain[None, :], table,
        proj_weight.reshape(ntp, ch, width),
    )

    hw = expert_gate.shape[2]
    sw = shared_gate.shape[1]
    nz = nsp // 2
    return pl.pallas_call(
        functools.partial(expert_kernel, nsp, ntp, cap),
        out_shape=jax.ShapeDtypeStruct((tok, width), BF16),
        in_specs=[vm] * 4 + [hbm] * 6,
        out_specs=vm,
        scratch_shapes=[
            VMEM((nsp, ntp, tok, width), BF16),
            VMEM((ntp, width, hw), BF16),
            VMEM((ntp, width, hw), BF16),
            VMEM((ntp, width, sw), BF16),
            VMEM((ntp, width, sw), BF16),
            VMEM((ntp, hw, width), BF16),
            VMEM((ntp, sw, width), BF16),
            VMEM((2, 2, tok, hw), F32),
            VMEM((nsp, ntp, cap, hw), BF16),
            VMEM((ntp, tok, sw), BF16),
            VMEM((nsp, cap, width), BF16),
            VMEM((nsp, cap, width), BF16),
            DMA((7,)),
            DMA((nsp, ntp, 2)),
            DMA((nz - 1, 2)),
            DMA((nz, 2)), DMA((nz, 2)), DMA((nz, 2)),
            DMA((nz, ntp, 2)),
            DMA((nsp, ntp - 1)), DMA((nsp, ntp - 1)),
            DMA((ntp - 1,)), DMA((ntp - 1,)),
            DMA((nsp,)), DMA((nsp,)),
        ],
        compiler_params=pltpu.CompilerParams(
            collective_id=2, has_side_effects=True, vmem_limit_bytes=56 << 20
        ),
        name="experts",
    )(
        normed, mid, route_all, poscol,
        expert_gate[0].reshape(ntp, width, hw),
        expert_up[0].reshape(ntp, width, hw),
        shared_gate.reshape(ntp, width, sw),
        shared_up.reshape(ntp, width, sw),
        expert_down[0].reshape(ntp, hw, width),
        shared_down.reshape(ntp, sw, width),
    )


def chosen(*args):
    tok, width = args[7].shape
    nsp = lax.axis_size("sp")
    ntp = lax.axis_size("tp")
    cap = 2 * tok * args[9].shape[1] // nsp
    fits = 2 * nsp * ntp * tok * width <= 16 << 20
    aligned = tok % 256 == 0 and width % 128 == 0 and cap % 128 == 0
    if ntp == 4 and nsp % 2 == 0 and fits and aligned:
        return fast_shards(*args)
    return shards(*args)


def solution(mesh):
    in_specs = (
        P("sp", "tp"),
        P("sp", "tp"),
        P(None, "tp"),
        P("tp"),
        P("tp"),
        P("tp"),
        P(None, "tp"),
        P("sp", "tp"),
        P("tp"),
        P("sp", None),
        P("sp", None),
        P("sp", None, "tp"),
        P("sp", None, "tp"),
        P("sp", None, "tp"),
        P(None, "tp"),
        P(None, "tp"),
        P(None, "tp"),
    )
    out_specs = P("sp", "tp")
    return jax.shard_map(chosen, mesh=mesh, in_specs=in_specs, out_specs=out_specs, check_vma=False)
```

```python
import functools

import jax
import jax.numpy as jnp
from jax import lax
from jax.experimental import pallas as pl
from jax.experimental.pallas import tpu as pltpu
from jax.sharding import PartitionSpec as P

D = 4096
CONV = 2048


norm_eps = 1e-06


def shifted(block, axis, distance):
    devices = range(lax.axis_size(axis))
    route = [(i - distance, i) for i in devices if i - distance in devices]
    return lax.ppermute(block, axis, route)


def shards(
    u_val,
    u_gate,
    conv_weight,
    conv_bias,
    ln_gain,
    ln_bias,
    proj_weight,
    resid,
    norm_gain,
    route_ids,
    route_wts,
    expert_gate,
    expert_up,
    expert_down,
    shared_gate,
    shared_up,
    shared_down,
):
    tok_rows = u_val.shape[0]
    sp_count = lax.axis_size("sp")
    tp_count = lax.axis_size("tp")
    kernel_width = conv_weight.shape[0]
    gated = (u_val.astype(jnp.float32) * jax.nn.sigmoid(u_gate.astype(jnp.float32))).astype(
        jnp.bfloat16
    )
    rim_rows = shifted(gated[tok_rows - (kernel_width - 1) :], "sp", 1)
    padded = lax.optimization_barrier(jnp.concatenate([rim_rows, gated], axis=0)).astype(
        jnp.float32
    )
    conv_sum = jnp.zeros((tok_rows, gated.shape[1]), jnp.float32) + conv_bias[None, :]
    for tap_index in range(kernel_width):
        conv_sum = (
            conv_sum + conv_weight[tap_index][None, :] * padded[tap_index : tap_index + tok_rows]
        )
    stat_sums = lax.psum((jnp.sum(conv_sum, axis=1), jnp.sum(conv_sum * conv_sum, axis=1)), "tp")
    channel_mean = stat_sums[0] / CONV
    channel_var = stat_sums[1] / CONV - channel_mean * channel_mean
    normed_conv = (conv_sum - channel_mean[:, None]) * lax.rsqrt(channel_var + norm_eps)[:, None]
    conv_out = jax.nn.silu(normed_conv * ln_gain + ln_bias).astype(jnp.bfloat16)
    projected = jnp.dot(
        lax.all_gather(conv_out, "tp", axis=1, tiled=True),
        proj_weight,
        preferred_element_type=jnp.float32,
    )
    residual_mid = (resid.astype(jnp.float32) + projected).astype(jnp.bfloat16)
    residual_wide = residual_mid.astype(jnp.float32)
    square_sum = lax.psum(jnp.sum(residual_wide * residual_wide, axis=1), "tp")
    normed_rows = (
        residual_wide * lax.rsqrt(square_sum / D + norm_eps)[:, None] * norm_gain
    ).astype(jnp.bfloat16)
    rows_full = lax.all_gather(normed_rows, "tp", axis=1, tiled=True)
    topk_count = route_ids.shape[1]
    capacity = 2 * tok_rows * topk_count // sp_count
    pair_ids = route_ids.reshape(-1)
    onehot = (pair_ids[:, None] == jnp.arange(sp_count, dtype=jnp.int32)[None, :]).astype(jnp.int32)
    before = jnp.cumsum(onehot, axis=0) - onehot
    position = jnp.sum(before * onehot, axis=1)
    pair_slot = pair_ids * capacity + position
    matches = (
        jnp.arange(sp_count * capacity, dtype=jnp.int32)[:, None] == pair_slot[None, :]
    ).astype(jnp.int32)
    pair_tok = jnp.arange(tok_rows * topk_count, dtype=jnp.int32) // topk_count
    filled = jnp.sum(matches, axis=1)
    slot_tok = jnp.sum(matches * pair_tok[None, :], axis=1) + (1 - filled) * tok_rows
    rows_ext = jnp.concatenate(
        [rows_full, jnp.zeros((1, rows_full.shape[1]), jnp.bfloat16)], axis=0
    )
    part_slots = capacity // tp_count
    tp_index = lax.axis_index("tp")
    local_slots = lax.dynamic_slice_in_dim(
        slot_tok.reshape(sp_count, capacity), tp_index * part_slots, part_slots, 1
    )
    send_rows = jnp.take(rows_ext, local_slots.reshape(-1), axis=0).reshape(
        sp_count, part_slots, -1
    )
    received = lax.all_to_all(send_rows, "sp", split_axis=0, concat_axis=0, tiled=True)
    arrived = lax.all_gather(received, "tp", axis=1, tiled=True)
    slot_rows = arrived.reshape(sp_count * capacity, -1)
    gate_pre = jnp.dot(slot_rows, expert_gate[0], preferred_element_type=jnp.float32)
    up_proj = jnp.dot(slot_rows, expert_up[0], preferred_element_type=jnp.float32)
    hidden = (jax.nn.silu(gate_pre) * up_proj).astype(jnp.bfloat16)
    shared_pre = jnp.dot(rows_full, shared_gate, preferred_element_type=jnp.float32)
    shared_upper = jnp.dot(rows_full, shared_up, preferred_element_type=jnp.float32)
    shared_hidden = (jax.nn.silu(shared_pre) * shared_upper).astype(jnp.bfloat16)
    out_cols = expert_down.shape[2]
    routed_rows = expert_down[0]
    routed_out = jnp.dot(
        lax.all_gather(hidden, "tp", axis=1, tiled=True),
        routed_rows,
        preferred_element_type=jnp.float32,
    )
    shared_out = jnp.dot(
        lax.all_gather(shared_hidden, "tp", axis=1, tiled=True),
        shared_down,
        preferred_element_type=jnp.float32,
    )
    expert_rows = routed_out.astype(jnp.bfloat16).reshape(sp_count, capacity, out_cols)
    returned_rows = lax.all_to_all(expert_rows, "sp", split_axis=0, concat_axis=0, tiled=True)
    returned_flat = returned_rows.reshape(sp_count * capacity, out_cols)
    picked = (
        jnp.take(returned_flat, pair_slot, axis=0)
        .astype(jnp.float32)
        .reshape(tok_rows, topk_count, out_cols)
    )
    routed = jnp.sum(picked * route_wts[:, :, None], axis=1)
    return (residual_wide + shared_out + routed).astype(jnp.bfloat16)


VMEM = pltpu.VMEM
DMA = pltpu.SemaphoreType.DMA
F32 = jnp.float32
BF16 = jnp.bfloat16


def rcopy(src, dst, send_sem, recv_sem, device):
    return pltpu.make_async_remote_copy(
        src_ref=src,
        dst_ref=dst,
        send_sem=send_sem,
        recv_sem=recv_sem,
        device_id=device,
        device_id_type=pl.DeviceIdType.MESH,
    )


def dot(a, b):
    return jnp.dot(a, b, preferred_element_type=F32)


def greet(nsp, ntp, me, t):
    barrier = pltpu.get_barrier_semaphore()
    for j in range(1, ntp):
        pl.semaphore_signal(
            barrier, inc=1, device_id=(me, (t + j) % ntp), device_id_type=pl.DeviceIdType.MESH
        )
    for j in range(1, nsp):
        pl.semaphore_signal(
            barrier, inc=1, device_id=((me + j) % nsp, t), device_id_type=pl.DeviceIdType.MESH
        )
    pl.semaphore_wait(barrier, ntp - 1 + nsp - 1)


def front_kernel(
    nsp, ntp,
    conv, gain, bias, resid, ngain, route, proj_hbm,
    normed, mid, route_all,
    proj, gbuf, st, st2, rbuf,
    lsem, gsend, grecv, ssend, srecv, s2send, s2recv, rsend, rrecv,
):
    me = lax.axis_index("sp")
    t = lax.axis_index("tp")
    tok = conv.shape[0]
    weights = pltpu.make_async_copy(proj_hbm, proj, lsem.at[0])
    weights.start()
    greet(nsp, ntp, me, t)
    tables = []
    for j in range(1, nsp):
        e = (me + j) % nsp
        copy = rcopy(route.at[e], rbuf.at[me], rsend.at[j - 1], rrecv.at[j - 1], (e, t))
        copy.start()
        tables.append(copy)
    rbuf[me] = route[me]

    def exchange(stat, columns, send, recv):
        lane = lax.broadcasted_iota(jnp.int32, (tok, 128), 1)
        packed = jnp.zeros((tok, 128), F32)
        for i, column in enumerate(columns):
            packed = packed + jnp.where(lane == i, column, 0.0)
        stat[t] = jnp.transpose(packed)[0:8, :]
        copies = []
        for j in range(1, ntp):
            copy = rcopy(
                stat.at[t], stat.at[t], send.at[j - 1], recv.at[j - 1], (me, (t + j) % ntp)
            )
            copy.start()
            copies.append(copy)
        for copy in copies:
            copy.wait()
        total = stat[0]
        for i in range(1, ntp):
            total = total + stat[i]
        return jnp.transpose(jnp.concatenate([total] * 16, axis=0))

    x = conv[...]
    sums = exchange(
        st,
        [jnp.sum(x, axis=1, keepdims=True), jnp.sum(x * x, axis=1, keepdims=True)],
        ssend,
        srecv,
    )
    channels = conv.shape[1] * ntp
    mean = sums[:, 0:1] / channels
    var = sums[:, 1:2] / channels - mean * mean
    v = (x - mean) * lax.rsqrt(var + norm_eps) * gain[...] + bias[...]
    gbuf[t] = (v / (1.0 + jnp.exp(-v))).astype(BF16)
    copies = []
    for j in range(1, ntp):
        copy = rcopy(gbuf.at[t], gbuf.at[t], gsend.at[j - 1], grecv.at[j - 1], (me, (t + j) % ntp))
        copy.start()
        copies.append(copy)
    weights.wait()
    total = resid[...].astype(F32) + dot(gbuf[t], proj[t])
    for j in range(1, ntp):
        copies[j - 1].wait_recv()
        q = (t - j + ntp) % ntp
        total = total + dot(gbuf[q], proj[q])
    mid[...] = total.astype(BF16)
    wide = mid[...].astype(F32)
    squares = exchange(st2, [jnp.sum(wide * wide, axis=1, keepdims=True)], s2send, s2recv)
    scale = lax.rsqrt(squares[:, 0:1] / (mid.shape[1] * ntp) + norm_eps)
    normed[...] = (wide * scale * ngain[...]).astype(BF16)
    for copy in copies:
        copy.wait_send()
    for copy in tables:
        copy.wait()
    route_all[...] = rbuf[...]


def expert_kernel(
    nsp, ntp, cap,
    normed, mid, route, poscol, wg_h, wu_h, sg_h, su_h, wd_h, sd_h,
    out,
    buf, wg, wu, sg, su, wd, sd, acc, hid, shid, osend, ret, total,
    lsem, recv, zsend, xsend, ysend, relay, dsend, hsend, hrecv, shsend, shrecv, osem, orecv,
):
    me = lax.axis_index("sp")
    t = lax.axis_index("tp")
    tok, width = normed.shape
    half = tok // 2
    hidden_width = wg.shape[2]
    nz = nsp // 2
    z = me // 2
    c = me % 2
    partner = me + 1 - 2 * c
    t1 = t + 1 - 2 * (t % 2)
    t2 = t + 2 - 4 * (t // 2)
    t3 = 3 - t
    loads = [
        pltpu.make_async_copy(a, b, lsem.at[i])
        for i, (a, b) in enumerate(
            [(wg_h, wg), (wu_h, wu), (sg_h, sg), (su_h, su), (wd_h, wd), (sd_h, sd)]
        )
    ]
    own = pltpu.make_async_copy(normed, buf.at[me, t], lsem.at[6])
    own.start()
    for load in loads:
        load.start()
    greet(nsp, ntp, me, t)
    own.wait()

    def rows(b, q, h):
        return buf.at[b, q, pl.ds(h * half, half)]

    def push(b, q, h, sem, device):
        return rcopy(rows(b, q, h), rows(b, q, h), sem, recv.at[b, q, h], device)

    def arrived(b, q, h):
        push(b, q, h, zsend.at[0, 0], (me, t1)).wait_recv()

    def spread(k, b):
        copies = []
        for h in range(2):
            copies.append(push(b, t, h, xsend.at[k, h], (me, t1)))
            copies.append(push(b, t, h, ysend.at[k, h], (me, t2)))
            copies.append(push(b, t, h, dsend.at[k, 0, h], (partner, t)))
        return copies

    def relays(k, b):
        return [
            push(b, t1, 0, relay.at[k, 0], (me, t2)),
            push(b, t2, 1, relay.at[k, 1], (me, t1)),
        ]

    def across(k, b, i, q, h):
        return push(b, q, h, dsend.at[k, i, h], (partner, t))

    far = []
    for k in range(1, nz):
        for h in range(2):
            far.append(push(me, t, h, zsend.at[k - 1, h], (2 * ((z + k) % nz) + c, t)))
    for copy in far:
        copy.start()
    for copy in spread(0, me):
        copy.start()
    def gate_up(i, b, q, first):
        data = buf[b, q]
        g = dot(data, wg[q])
        u = dot(data, wu[q])
        if first:
            acc[i, 0] = g
            acc[i, 1] = u
        else:
            acc[i, 0] += g
            acc[i, 1] += u

    def selection(b):
        slot = lax.broadcasted_iota(jnp.int32, (cap, tok), 0).astype(F32)
        return jnp.where(slot == route[b, 0:1, :], 1.0, 0.0)

    def gather(ref, part, send, arrive):
        size = part // 2

        def piece(q, h, sem, device):
            block = ref.at[q, pl.ds(h * size, size)]
            return rcopy(block, block, sem, arrive.at[q, h], device)

        first = [
            piece(t, h, send.at[i, h], (me, peer))
            for h in range(2)
            for i, peer in enumerate((t1, t2))
        ]
        second = [piece(t1, 0, send.at[2, 0], (me, t2)), piece(t2, 1, send.at[2, 1], (me, t1))]

        def wait(q, h):
            piece(q, h, send.at[0, 0], (me, t1)).wait_recv()

        def forward():
            wait(t1, 0)
            second[0].start()
            wait(t2, 1)
            second[1].start()

        def finish():
            wait(t1, 1)
            wait(t2, 0)
            wait(t3, 0)
            wait(t3, 1)

        return first, second, forward, finish

    def hidden_gather(b):
        return gather(hid.at[b], cap, hsend.at[b], hrecv.at[b])

    shared_gather = gather(shid, tok, shsend, shrecv)

    def gated(g, u):
        return (g / (1.0 + jnp.exp(-g)) * u).astype(BF16)

    def finish(i, b):
        hs = dot(selection(b).astype(BF16), gated(acc[i, 0], acc[i, 1]))
        hid[b, t] = hs.astype(BF16)

    def home(b):
        return rcopy(osend.at[b], ret.at[me], osem.at[b], orecv.at[me], (b, t))

    def down(b):
        hidden_gather(b)[3]()
        o = dot(hid[b, 0], wd[0])
        for q in range(1, ntp):
            o = o + dot(hid[b, q], wd[q])
        weight = jnp.sum(selection(b) * route[b, 1:2, :], axis=1, keepdims=True)
        return (o * weight).astype(BF16)

    def step(k, carry):
        zk = (z - k + nz) % nz

        @pl.when(k < nz)
        def _():
            b = 2 * zk + c
            pb = 2 * zk + 1 - c
            forward = relays(k, b)
            for h in range(2):
                arrived(b, t1, h)
                if h == 0:
                    forward[0].start()
                across(k, b, 1, t1, h).start()
            for h in range(2):
                arrived(b, t2, h)
                if h == 1:
                    forward[1].start()
                across(k, b, 2, t2, h).start()

        @pl.when(k > 1)
        def _():
            def one(i, state):
                hidden_gather(2 * ((z - k + 1 + nz) % nz) + i)[2]()
                return state

            lax.fori_loop(0, 2, one, 0)

        @pl.when(k < nz)
        def _():
            b = 2 * zk + c
            pb = 2 * zk + 1 - c

            @pl.when(k < nz - 1)
            def _():
                bn = 2 * ((z - k - 1 + nz) % nz) + c
                for h in range(2):
                    arrived(bn, t, h)
                for copy in spread(k + 1, bn):
                    copy.start()

            @pl.when(k == 0)
            def _():
                loads[0].wait()
                loads[1].wait()

            gate_up(0, b, t, True)
            gate_up(0, b, t1, False)
            gate_up(0, b, t2, False)
            for i, q in enumerate((t, t1, t2)):
                for h in range(2):
                    arrived(pb, q, h)
                gate_up(1, pb, q, i == 0)
        @pl.when(k == 2)
        def _():
            loads[4].wait()
            loads[5].wait()

        @pl.when(k > 1)
        def _():
            zp = (z - k + 1 + nz) % nz

            def one(i, state):
                b = 2 * zp + i
                osend[b] = down(b)
                home(b).start()
                return state

            lax.fori_loop(0, 2, one, 0)

        @pl.when(k < nz)
        def _():
            b = 2 * zk + c
            pb = 2 * zk + 1 - c
            for h in range(2):
                arrived(b, t3, h)
                across(k, b, 3, t3, h).start()
            gate_up(0, b, t3, False)
            finish(0, b)
            for h in range(2):
                arrived(pb, t3, h)
            gate_up(1, pb, t3, False)
            finish(1, pb)

            @pl.when(k > 0)
            def _():
                for copy in hidden_gather(b)[0] + hidden_gather(pb)[0]:
                    copy.start()

            @pl.when(k == nz - 1)
            def _():
                for copy in hidden_gather(me)[0] + hidden_gather(partner)[0] + shared_gather[0]:
                    copy.start()

        @pl.when(k == 0)
        def _():
            def quarter(q, state):
                data = buf[me, q]
                g = dot(data, sg[q])
                u = dot(data, su[q])
                acc[0, 0] = jnp.where(q == 0, g, acc[0, 0] + g)
                acc[0, 1] = jnp.where(q == 0, u, acc[0, 1] + u)
                return state

            loads[2].wait()
            loads[3].wait()
            lax.fori_loop(0, ntp, quarter, 0)
            shid[t] = gated(acc[0, 0], acc[0, 1])

        return carry

    lax.fori_loop(0, nz + 1, step, 0)

    hidden_gather(me)[2]()
    hidden_gather(partner)[2]()
    shared_gather[2]()
    osend[partner] = down(partner)
    home(partner).start()
    ret[me] = down(me)
    shared_gather[3]()
    o = dot(shid[0], sd[0])
    for q in range(1, ntp):
        o = o + dot(shid[q], sd[q])
    total[...] = mid[...].astype(F32) + o

    for copy in shared_gather[0] + shared_gather[1]:
        copy.wait_send()

    def drain(k, carry):
        b = 2 * ((z - k + nz) % nz) + c
        for copy in spread(k, b) + relays(k, b):
            copy.wait_send()
        for i, q in ((1, t1), (2, t2), (3, t3)):
            for h in range(2):
                across(k, b, i, q, h).wait_send()
        return carry

    lax.fori_loop(0, nz, drain, 0)
    for copy in far:
        copy.wait_send()

    def drain_hidden(b, carry):
        for copy in hidden_gather(b)[0] + hidden_gather(b)[1]:
            copy.wait_send()
        return carry

    lax.fori_loop(0, nsp, drain_hidden, 0)
    for j in range(1, nsp):
        e = (me + j) % nsp
        rcopy(osend.at[e], ret.at[e], osem.at[e], orecv.at[e], (e, t)).wait()
    lane = lax.broadcasted_iota(jnp.int32, (tok, cap), 1).astype(F32)
    result = total[...]
    for e in range(nsp):
        pick = jnp.where(lane == poscol[:, e : e + 1], 1.0, 0.0).astype(BF16)
        result = result + dot(pick, ret[e])
    out[...] = result.astype(BF16)


def fast_shards(
    u_val, u_gate, conv_weight, conv_bias, ln_gain, ln_bias, proj_weight, resid, norm_gain,
    route_ids, route_wts, expert_gate, expert_up, expert_down, shared_gate, shared_up, shared_down,
):
    tok = u_val.shape[0]
    nsp = lax.axis_size("sp")
    ntp = lax.axis_size("tp")
    taps = conv_weight.shape[0]
    gated = (u_val.astype(F32) * jax.nn.sigmoid(u_gate.astype(F32))).astype(BF16)
    rim = shifted(gated[tok - (taps - 1) :], "sp", 1)
    padded = lax.optimization_barrier(jnp.concatenate([rim, gated], axis=0)).astype(F32)
    conv_sum = jnp.zeros((tok, gated.shape[1]), F32) + conv_bias[None, :]
    for i in range(taps):
        conv_sum = conv_sum + conv_weight[i][None, :] * padded[i : i + tok]

    top = route_ids.shape[1]
    cap = 2 * tok * top // nsp
    experts = jnp.arange(nsp, dtype=jnp.int32)
    named = jnp.zeros((nsp, tok), F32)
    weight = jnp.zeros((nsp, tok), F32)
    for k in range(top):
        hit = route_ids[:, k][None, :] == experts[:, None]
        named = named + hit.astype(F32)
        weight = weight + jnp.where(hit, route_wts[:, k][None, :], 0.0)
    earlier = (jnp.arange(tok)[:, None] < jnp.arange(tok)[None, :]).astype(BF16)
    pos = jnp.where(named > 0, dot(named.astype(BF16), earlier), -1.0)
    table = jnp.concatenate(
        [pos[:, None, :], weight[:, None, :], jnp.zeros((nsp, 6, tok), F32)], axis=1
    )
    poscol = jnp.concatenate([pos.T, jnp.full((tok, 128 - nsp), -1.0, F32)], axis=1)

    ch = conv_sum.shape[1]
    width = resid.shape[1]
    vm = pl.BlockSpec(memory_space=VMEM)
    hbm = pl.BlockSpec(memory_space=pl.ANY)
    normed, mid, route_all = pl.pallas_call(
        functools.partial(front_kernel, nsp, ntp),
        out_shape=[
            jax.ShapeDtypeStruct((tok, width), BF16),
            jax.ShapeDtypeStruct((tok, width), BF16),
            jax.ShapeDtypeStruct((nsp, 8, tok), F32),
        ],
        in_specs=[vm] * 6 + [hbm],
        out_specs=[vm] * 3,
        scratch_shapes=[
            VMEM((ntp, ch, width), BF16),
            VMEM((ntp, tok, ch), BF16),
            VMEM((ntp, 8, tok), F32),
            VMEM((ntp, 8, tok), F32),
            VMEM((nsp, 8, tok), F32),
            DMA((1,)),
            DMA((ntp - 1,)), DMA((ntp - 1,)),
            DMA((ntp - 1,)), DMA((ntp - 1,)),
            DMA((ntp - 1,)), DMA((ntp - 1,)),
            DMA((nsp - 1,)), DMA((nsp - 1,)),
        ],
        compiler_params=pltpu.CompilerParams(
            collective_id=1, has_side_effects=True, vmem_limit_bytes=24 << 20
        ),
        name="front",
    )(
        conv_sum, ln_gain[None, :], ln_bias[None, :], resid, norm_gain[None, :], table,
        proj_weight.reshape(ntp, ch, width),
    )

    hw = expert_gate.shape[2]
    sw = shared_gate.shape[1]
    nz = nsp // 2
    return pl.pallas_call(
        functools.partial(expert_kernel, nsp, ntp, cap),
        out_shape=jax.ShapeDtypeStruct((tok, width), BF16),
        in_specs=[vm] * 4 + [hbm] * 6,
        out_specs=vm,
        scratch_shapes=[
            VMEM((nsp, ntp, tok, width), BF16),
            VMEM((ntp, width, hw), BF16),
            VMEM((ntp, width, hw), BF16),
            VMEM((ntp, width, sw), BF16),
            VMEM((ntp, width, sw), BF16),
            VMEM((ntp, hw, width), BF16),
            VMEM((ntp, sw, width), BF16),
            VMEM((2, 2, tok, hw), F32),
            VMEM((nsp, ntp, cap, hw), BF16),
            VMEM((ntp, tok, sw), BF16),
            VMEM((nsp, cap, width), BF16),
            VMEM((nsp, cap, width), BF16),
            VMEM((tok, width), F32),
            DMA((7,)),
            DMA((nsp, ntp, 2)),
            DMA((nz - 1, 2)),
            DMA((nz, 2)), DMA((nz, 2)), DMA((nz, 2)),
            DMA((nz, ntp, 2)),
            DMA((nsp, 3, 2)), DMA((nsp, ntp, 2)),
            DMA((3, 2)), DMA((ntp, 2)),
            DMA((nsp,)), DMA((nsp,)),
        ],
        compiler_params=pltpu.CompilerParams(
            collective_id=2, has_side_effects=True, vmem_limit_bytes=56 << 20
        ),
        name="experts",
    )(
        normed, mid, route_all, poscol,
        expert_gate[0].reshape(ntp, width, hw),
        expert_up[0].reshape(ntp, width, hw),
        shared_gate.reshape(ntp, width, sw),
        shared_up.reshape(ntp, width, sw),
        expert_down[0].reshape(ntp, hw, width),
        shared_down.reshape(ntp, sw, width),
    )


def chosen(*args):
    tok, width = args[7].shape
    nsp = lax.axis_size("sp")
    ntp = lax.axis_size("tp")
    cap = 2 * tok * args[9].shape[1] // nsp
    fits = 2 * nsp * ntp * tok * width <= 16 << 20
    aligned = tok % 256 == 0 and width % 128 == 0 and cap % 128 == 0
    if ntp == 4 and nsp % 2 == 0 and fits and aligned:
        return fast_shards(*args)
    return shards(*args)


def solution(mesh):
    in_specs = (
        P("sp", "tp"),
        P("sp", "tp"),
        P(None, "tp"),
        P("tp"),
        P("tp"),
        P("tp"),
        P(None, "tp"),
        P("sp", "tp"),
        P("tp"),
        P("sp", None),
        P("sp", None),
        P("sp", None, "tp"),
        P("sp", None, "tp"),
        P("sp", None, "tp"),
        P(None, "tp"),
        P(None, "tp"),
        P(None, "tp"),
    )
    out_specs = P("sp", "tp")
    return jax.shard_map(chosen, mesh=mesh, in_specs=in_specs, out_specs=out_specs, check_vma=False)
```

```python
import functools

import jax
import jax.numpy as jnp
from jax import lax
from jax.experimental import pallas as pl
from jax.experimental.pallas import tpu as pltpu
from jax.sharding import PartitionSpec as P

D = 4096
CONV = 2048


norm_eps = 1e-06


def shifted(block, axis, distance):
    devices = range(lax.axis_size(axis))
    route = [(i - distance, i) for i in devices if i - distance in devices]
    return lax.ppermute(block, axis, route)


def shards(
    u_val,
    u_gate,
    conv_weight,
    conv_bias,
    ln_gain,
    ln_bias,
    proj_weight,
    resid,
    norm_gain,
    route_ids,
    route_wts,
    expert_gate,
    expert_up,
    expert_down,
    shared_gate,
    shared_up,
    shared_down,
):
    tok_rows = u_val.shape[0]
    sp_count = lax.axis_size("sp")
    tp_count = lax.axis_size("tp")
    kernel_width = conv_weight.shape[0]
    gated = (u_val.astype(jnp.float32) * jax.nn.sigmoid(u_gate.astype(jnp.float32))).astype(
        jnp.bfloat16
    )
    rim_rows = shifted(gated[tok_rows - (kernel_width - 1) :], "sp", 1)
    padded = lax.optimization_barrier(jnp.concatenate([rim_rows, gated], axis=0)).astype(
        jnp.float32
    )
    conv_sum = jnp.zeros((tok_rows, gated.shape[1]), jnp.float32) + conv_bias[None, :]
    for tap_index in range(kernel_width):
        conv_sum = (
            conv_sum + conv_weight[tap_index][None, :] * padded[tap_index : tap_index + tok_rows]
        )
    stat_sums = lax.psum((jnp.sum(conv_sum, axis=1), jnp.sum(conv_sum * conv_sum, axis=1)), "tp")
    channel_mean = stat_sums[0] / CONV
    channel_var = stat_sums[1] / CONV - channel_mean * channel_mean
    normed_conv = (conv_sum - channel_mean[:, None]) * lax.rsqrt(channel_var + norm_eps)[:, None]
    conv_out = jax.nn.silu(normed_conv * ln_gain + ln_bias).astype(jnp.bfloat16)
    projected = jnp.dot(
        lax.all_gather(conv_out, "tp", axis=1, tiled=True),
        proj_weight,
        preferred_element_type=jnp.float32,
    )
    residual_mid = (resid.astype(jnp.float32) + projected).astype(jnp.bfloat16)
    residual_wide = residual_mid.astype(jnp.float32)
    square_sum = lax.psum(jnp.sum(residual_wide * residual_wide, axis=1), "tp")
    normed_rows = (
        residual_wide * lax.rsqrt(square_sum / D + norm_eps)[:, None] * norm_gain
    ).astype(jnp.bfloat16)
    rows_full = lax.all_gather(normed_rows, "tp", axis=1, tiled=True)
    topk_count = route_ids.shape[1]
    capacity = 2 * tok_rows * topk_count // sp_count
    pair_ids = route_ids.reshape(-1)
    onehot = (pair_ids[:, None] == jnp.arange(sp_count, dtype=jnp.int32)[None, :]).astype(jnp.int32)
    before = jnp.cumsum(onehot, axis=0) - onehot
    position = jnp.sum(before * onehot, axis=1)
    pair_slot = pair_ids * capacity + position
    matches = (
        jnp.arange(sp_count * capacity, dtype=jnp.int32)[:, None] == pair_slot[None, :]
    ).astype(jnp.int32)
    pair_tok = jnp.arange(tok_rows * topk_count, dtype=jnp.int32) // topk_count
    filled = jnp.sum(matches, axis=1)
    slot_tok = jnp.sum(matches * pair_tok[None, :], axis=1) + (1 - filled) * tok_rows
    rows_ext = jnp.concatenate(
        [rows_full, jnp.zeros((1, rows_full.shape[1]), jnp.bfloat16)], axis=0
    )
    part_slots = capacity // tp_count
    tp_index = lax.axis_index("tp")
    local_slots = lax.dynamic_slice_in_dim(
        slot_tok.reshape(sp_count, capacity), tp_index * part_slots, part_slots, 1
    )
    send_rows = jnp.take(rows_ext, local_slots.reshape(-1), axis=0).reshape(
        sp_count, part_slots, -1
    )
    received = lax.all_to_all(send_rows, "sp", split_axis=0, concat_axis=0, tiled=True)
    arrived = lax.all_gather(received, "tp", axis=1, tiled=True)
    slot_rows = arrived.reshape(sp_count * capacity, -1)
    gate_pre = jnp.dot(slot_rows, expert_gate[0], preferred_element_type=jnp.float32)
    up_proj = jnp.dot(slot_rows, expert_up[0], preferred_element_type=jnp.float32)
    hidden = (jax.nn.silu(gate_pre) * up_proj).astype(jnp.bfloat16)
    shared_pre = jnp.dot(rows_full, shared_gate, preferred_element_type=jnp.float32)
    shared_upper = jnp.dot(rows_full, shared_up, preferred_element_type=jnp.float32)
    shared_hidden = (jax.nn.silu(shared_pre) * shared_upper).astype(jnp.bfloat16)
    out_cols = expert_down.shape[2]
    routed_rows = expert_down[0]
    routed_out = jnp.dot(
        lax.all_gather(hidden, "tp", axis=1, tiled=True),
        routed_rows,
        preferred_element_type=jnp.float32,
    )
    shared_out = jnp.dot(
        lax.all_gather(shared_hidden, "tp", axis=1, tiled=True),
        shared_down,
        preferred_element_type=jnp.float32,
    )
    expert_rows = routed_out.astype(jnp.bfloat16).reshape(sp_count, capacity, out_cols)
    returned_rows = lax.all_to_all(expert_rows, "sp", split_axis=0, concat_axis=0, tiled=True)
    returned_flat = returned_rows.reshape(sp_count * capacity, out_cols)
    picked = (
        jnp.take(returned_flat, pair_slot, axis=0)
        .astype(jnp.float32)
        .reshape(tok_rows, topk_count, out_cols)
    )
    routed = jnp.sum(picked * route_wts[:, :, None], axis=1)
    return (residual_wide + shared_out + routed).astype(jnp.bfloat16)


VMEM = pltpu.VMEM
DMA = pltpu.SemaphoreType.DMA
F32 = jnp.float32
BF16 = jnp.bfloat16


def rcopy(src, dst, send_sem, recv_sem, device):
    return pltpu.make_async_remote_copy(
        src_ref=src,
        dst_ref=dst,
        send_sem=send_sem,
        recv_sem=recv_sem,
        device_id=device,
        device_id_type=pl.DeviceIdType.MESH,
    )


def dot(a, b):
    return jnp.dot(a, b, preferred_element_type=F32)


def greet(nsp, ntp, me, t):
    barrier = pltpu.get_barrier_semaphore()
    for j in range(1, ntp):
        pl.semaphore_signal(
            barrier, inc=1, device_id=(me, (t + j) % ntp), device_id_type=pl.DeviceIdType.MESH
        )
    for j in range(1, nsp):
        pl.semaphore_signal(
            barrier, inc=1, device_id=((me + j) % nsp, t), device_id_type=pl.DeviceIdType.MESH
        )
    return barrier, ntp - 1 + nsp - 1


def gather(me, t, ref, part, send, arrive):
    size = part // 2
    t1 = t + 1 - 2 * (t % 2)
    t2 = t + 2 - 4 * (t // 2)
    t3 = 3 - t

    def piece(q, h, sem, device):
        block = ref.at[q, pl.ds(h * size, size)]
        return rcopy(block, block, sem, arrive.at[q, h], device)

    first = [
        piece(t, h, send.at[i, h], (me, peer))
        for h in range(2)
        for i, peer in enumerate((t1, t2))
    ]
    second = [piece(t1, 0, send.at[2, 0], (me, t2)), piece(t2, 1, send.at[2, 1], (me, t1))]

    def wait(q, h):
        piece(q, h, send.at[0, 0], (me, t1)).wait_recv()

    def forward():
        wait(t1, 0)
        second[0].start()
        wait(t2, 1)
        second[1].start()

    def finish():
        wait(t1, 1)
        wait(t2, 0)
        wait(t3, 0)
        wait(t3, 1)

    return first, second, forward, finish


def front_kernel(
    nsp, ntp,
    conv, gain, bias, resid, ngain, route,
    normed, mid, weights, proj, gbuf, st, st2, rbuf,
    gsend, grecv, ssend, srecv, s2send, s2recv, rsend, rrecv,
):
    me = lax.axis_index("sp")
    t = lax.axis_index("tp")
    tok = conv.shape[0]
    tables = []
    for j in range(1, nsp):
        e = (me + j) % nsp
        copy = rcopy(route.at[e], rbuf.at[me], rsend.at[j - 1], rrecv.at[j - 1], (e, t))
        copy.start()
        tables.append(copy)
    rbuf[me] = route[me]

    def exchange(stat, columns, send, recv):
        lane = lax.broadcasted_iota(jnp.int32, (tok, 128), 1)
        packed = jnp.zeros((tok, 128), F32)
        for i, column in enumerate(columns):
            packed = packed + jnp.where(lane == i, column, 0.0)
        stat[t] = jnp.transpose(packed)[0:8, :]
        copies = []
        for j in range(1, ntp):
            copy = rcopy(
                stat.at[t], stat.at[t], send.at[j - 1], recv.at[j - 1], (me, (t + j) % ntp)
            )
            copy.start()
            copies.append(copy)
        for copy in copies:
            copy.wait()
        total = stat[0]
        for i in range(1, ntp):
            total = total + stat[i]
        return jnp.transpose(jnp.concatenate([total] * 16, axis=0))

    x = conv[...]
    sums = exchange(
        st,
        [jnp.sum(x, axis=1, keepdims=True), jnp.sum(x * x, axis=1, keepdims=True)],
        ssend,
        srecv,
    )
    channels = conv.shape[1] * ntp
    mean = sums[:, 0:1] / channels
    var = sums[:, 1:2] / channels - mean * mean
    v = (x - mean) * lax.rsqrt(var + norm_eps) * gain[...] + bias[...]
    gbuf[t] = (v / (1.0 + jnp.exp(-v))).astype(BF16)
    first, second, forward, settle = gather(me, t, gbuf, tok, gsend, grecv)
    for copy in first:
        copy.start()
    weights.wait()
    total = resid[...].astype(F32) + dot(gbuf[t], proj[t])
    forward()
    settle()
    for i in (1, 2, 3):
        q = (t + i) % ntp
        total = total + dot(gbuf[q], proj[q])
    mid[...] = total.astype(BF16)
    wide = mid[...].astype(F32)
    squares = exchange(st2, [jnp.sum(wide * wide, axis=1, keepdims=True)], s2send, s2recv)
    scale = lax.rsqrt(squares[:, 0:1] / (mid.shape[1] * ntp) + norm_eps)
    normed[...] = (wide * scale * ngain[...]).astype(BF16)
    for copy in first + second:
        copy.wait_send()
    for copy in tables:
        copy.wait()


def expert_kernel(
    nsp, ntp, cap,
    normed, mid, route, poscol, loads, out,
    buf, wg, wu, sg, su, wd, sd, acc, hid, shid, osend, ret, total,
    osem_own, recv, zsend, xsend, ysend, relay, dsend, hsend, hrecv, shsend, shrecv, osem, orecv,
):
    me = lax.axis_index("sp")
    t = lax.axis_index("tp")
    tok, width = normed.shape
    half = tok // 2
    hidden_width = wg.shape[2]
    nz = nsp // 2
    z = me // 2
    c = me % 2
    partner = me + 1 - 2 * c
    t1 = t + 1 - 2 * (t % 2)
    t2 = t + 2 - 4 * (t // 2)
    t3 = 3 - t
    own = pltpu.make_async_copy(normed, buf.at[me, t], osem_own.at[0])
    own.start()
    own.wait()

    def rows(b, q, h):
        return buf.at[b, q, pl.ds(h * half, half)]

    def push(b, q, h, sem, device):
        return rcopy(rows(b, q, h), rows(b, q, h), sem, recv.at[b, q, h], device)

    def arrived(b, q, h):
        push(b, q, h, zsend.at[0, 0], (me, t1)).wait_recv()

    def spread(k, b):
        copies = []
        for h in range(2):
            copies.append(push(b, t, h, xsend.at[k, h], (me, t1)))
            copies.append(push(b, t, h, ysend.at[k, h], (me, t2)))
            copies.append(push(b, t, h, dsend.at[k, 0, h], (partner, t)))
        return copies

    def relays(k, b):
        return [
            push(b, t1, 0, relay.at[k, 0], (me, t2)),
            push(b, t2, 1, relay.at[k, 1], (me, t1)),
        ]

    def across(k, b, i, q, h):
        return push(b, q, h, dsend.at[k, i, h], (partner, t))

    far = []
    for k in range(1, nz):
        for h in range(2):
            far.append(push(me, t, h, zsend.at[k - 1, h], (2 * ((z + k) % nz) + c, t)))
    for copy in far:
        copy.start()
    for copy in spread(0, me):
        copy.start()
    def gate_up(i, b, q, first):
        data = buf[b, q]
        g = dot(data, wg[q])
        u = dot(data, wu[q])
        if first:
            acc[i, 0] = g
            acc[i, 1] = u
        else:
            acc[i, 0] += g
            acc[i, 1] += u

    def selection(b):
        slot = lax.broadcasted_iota(jnp.int32, (cap, tok), 0).astype(F32)
        return jnp.where(slot == route[b, 0:1, :], 1.0, 0.0)

    def hidden_gather(b):
        return gather(me, t, hid.at[b], cap, hsend.at[b], hrecv.at[b])

    shared_gather = gather(me, t, shid, tok, shsend, shrecv)

    def gated(g, u):
        return (g / (1.0 + jnp.exp(-g)) * u).astype(BF16)

    def finish(i, b):
        hs = dot(selection(b).astype(BF16), gated(acc[i, 0], acc[i, 1]))
        hid[b, t] = hs.astype(BF16)

    def home(b):
        return rcopy(osend.at[b], ret.at[me], osem.at[b], orecv.at[me], (b, t))

    def down(b):
        hidden_gather(b)[3]()
        o = dot(hid[b, 0], wd[0])
        for q in range(1, ntp):
            o = o + dot(hid[b, q], wd[q])
        weight = jnp.sum(selection(b) * route[b, 1:2, :], axis=1, keepdims=True)
        return (o * weight).astype(BF16)

    def step(k, carry):
        zk = (z - k + nz) % nz

        @pl.when(k < nz)
        def _():
            b = 2 * zk + c
            pb = 2 * zk + 1 - c
            forward = relays(k, b)
            for h in range(2):
                arrived(b, t1, h)
                if h == 0:
                    forward[0].start()
                across(k, b, 1, t1, h).start()
            for h in range(2):
                arrived(b, t2, h)
                if h == 1:
                    forward[1].start()
                across(k, b, 2, t2, h).start()

        @pl.when(k > 1)
        def _():
            def one(i, state):
                hidden_gather(2 * ((z - k + 1 + nz) % nz) + i)[2]()
                return state

            lax.fori_loop(0, 2, one, 0)

        @pl.when(k == nz)
        def _():
            for copy in hidden_gather(me)[0] + hidden_gather(partner)[0] + shared_gather[0]:
                copy.start()

        @pl.when(k < nz)
        def _():
            b = 2 * zk + c
            pb = 2 * zk + 1 - c

            @pl.when(k < nz - 1)
            def _():
                bn = 2 * ((z - k - 1 + nz) % nz) + c
                for h in range(2):
                    arrived(bn, t, h)
                for copy in spread(k + 1, bn):
                    copy.start()

            @pl.when(k == 0)
            def _():
                loads[0].wait()
                loads[1].wait()

            gate_up(0, b, t, True)
            gate_up(0, b, t1, False)
            gate_up(0, b, t2, False)
            for i, q in enumerate((t, t1, t2)):
                for h in range(2):
                    arrived(pb, q, h)
                gate_up(1, pb, q, i == 0)
        @pl.when(k == 2)
        def _():
            loads[4].wait()
            loads[5].wait()

        @pl.when(k > 1)
        def _():
            zp = (z - k + 1 + nz) % nz

            def one(i, state):
                b = 2 * zp + i
                osend[b] = down(b)
                home(b).start()
                return state

            lax.fori_loop(0, 2, one, 0)

        @pl.when(k < nz)
        def _():
            b = 2 * zk + c
            pb = 2 * zk + 1 - c
            for h in range(2):
                arrived(b, t3, h)
                across(k, b, 3, t3, h).start()
            gate_up(0, b, t3, False)
            finish(0, b)

            @pl.when(k > 0)
            def _():
                for copy in hidden_gather(b)[0]:
                    copy.start()

            for h in range(2):
                arrived(pb, t3, h)
            gate_up(1, pb, t3, False)
            finish(1, pb)

            @pl.when(k > 0)
            def _():
                for copy in hidden_gather(pb)[0]:
                    copy.start()

        @pl.when(k == 0)
        def _():
            def quarter(q, state):
                data = buf[me, q]
                g = dot(data, sg[q])
                u = dot(data, su[q])
                acc[0, 0] = jnp.where(q == 0, g, acc[0, 0] + g)
                acc[0, 1] = jnp.where(q == 0, u, acc[0, 1] + u)
                return state

            loads[2].wait()
            loads[3].wait()
            lax.fori_loop(0, ntp, quarter, 0)
            shid[t] = gated(acc[0, 0], acc[0, 1])

        return carry

    lax.fori_loop(0, nz + 1, step, 0)

    hidden_gather(me)[2]()
    hidden_gather(partner)[2]()
    shared_gather[2]()
    osend[partner] = down(partner)
    home(partner).start()
    ret[me] = down(me)
    shared_gather[3]()
    o = dot(shid[0], sd[0])
    for q in range(1, ntp):
        o = o + dot(shid[q], sd[q])
    total[...] = mid[...].astype(F32) + o

    for copy in shared_gather[0] + shared_gather[1]:
        copy.wait_send()

    def drain(k, carry):
        b = 2 * ((z - k + nz) % nz) + c
        for copy in spread(k, b) + relays(k, b):
            copy.wait_send()
        for i, q in ((1, t1), (2, t2), (3, t3)):
            for h in range(2):
                across(k, b, i, q, h).wait_send()
        return carry

    lax.fori_loop(0, nz, drain, 0)
    for copy in far:
        copy.wait_send()

    def drain_hidden(b, carry):
        for copy in hidden_gather(b)[0] + hidden_gather(b)[1]:
            copy.wait_send()
        return carry

    lax.fori_loop(0, nsp, drain_hidden, 0)
    for j in range(1, nsp):
        e = (me + j) % nsp
        rcopy(osend.at[e], ret.at[e], osem.at[e], orecv.at[e], (e, t)).wait()
    lane = lax.broadcasted_iota(jnp.int32, (tok, cap), 1).astype(F32)
    result = total[...]
    for e in range(nsp):
        pick = jnp.where(lane == poscol[:, e : e + 1], 1.0, 0.0).astype(BF16)
        result = result + dot(pick, ret[e])
    out[...] = result.astype(BF16)


def convolve(padded, taps, bias, conv):
    tok, ch = conv.shape
    block = 64
    for r in range(0, tok, block):
        for l in range(0, ch, 128):
            total = jnp.zeros((block, 128), F32) + bias[:, l : l + 128]
            for i in range(taps.shape[0]):
                rows = padded[r + i : r + i + block, l : l + 128]
                total = total + taps[i : i + 1, l : l + 128] * rows
            conv[r : r + block, l : l + 128] = total


def layer_kernel(
    nsp, ntp, cap,
    padded, taps, tap_bias, gain, bias, resid, ngain, table, poscol,
    proj_h, wg_h, wu_h, sg_h, su_h, wd_h, sd_h,
    out,
    lsem, conv, normed, mid, rbuf, proj, gbuf, st, st2, *rest,
):
    front_sems = rest[:8]
    rest = rest[8:]
    pairs = zip((proj_h, wg_h, wu_h, sg_h, su_h, wd_h, sd_h), (proj,) + tuple(rest[1:7]))
    loads = [pltpu.make_async_copy(a, b, lsem.at[i]) for i, (a, b) in enumerate(pairs)]
    for load in loads:
        load.start()
    barrier, count = greet(nsp, ntp, lax.axis_index("sp"), lax.axis_index("tp"))
    convolve(padded, taps, tap_bias, conv)
    pl.semaphore_wait(barrier, count)
    front_kernel(
        nsp, ntp, conv, gain, bias, resid, ngain, table,
        normed, mid, loads[0], proj, gbuf, st, st2, rbuf, *front_sems,
    )
    expert_kernel(nsp, ntp, cap, normed, mid, rbuf, poscol, loads[1:], out, *rest)


def fast_shards(
    u_val, u_gate, conv_weight, conv_bias, ln_gain, ln_bias, proj_weight, resid, norm_gain,
    route_ids, route_wts, expert_gate, expert_up, expert_down, shared_gate, shared_up, shared_down,
):
    tok = u_val.shape[0]
    nsp = lax.axis_size("sp")
    ntp = lax.axis_size("tp")
    taps = conv_weight.shape[0]
    gated = (u_val.astype(F32) * jax.nn.sigmoid(u_gate.astype(F32))).astype(BF16)
    rim = shifted(gated[tok - (taps - 1) :], "sp", 1)
    spare = -(tok + taps - 1) % 8
    padded = jnp.concatenate(
        [rim, gated, jnp.zeros((spare, gated.shape[1]), BF16)], axis=0
    ).astype(F32)
    ch = gated.shape[1]

    top = route_ids.shape[1]
    cap = 2 * tok * top // nsp
    experts = jnp.arange(nsp, dtype=jnp.int32)
    named = jnp.zeros((nsp, tok), F32)
    weight = jnp.zeros((nsp, tok), F32)
    for k in range(top):
        hit = route_ids[:, k][None, :] == experts[:, None]
        named = named + hit.astype(F32)
        weight = weight + jnp.where(hit, route_wts[:, k][None, :], 0.0)
    earlier = (jnp.arange(tok)[:, None] < jnp.arange(tok)[None, :]).astype(BF16)
    pos = jnp.where(named > 0, dot(named.astype(BF16), earlier), -1.0)
    table = jnp.concatenate(
        [pos[:, None, :], weight[:, None, :], jnp.zeros((nsp, 6, tok), F32)], axis=1
    )
    poscol = jnp.concatenate([pos.T, jnp.full((tok, 128 - nsp), -1.0, F32)], axis=1)

    width = resid.shape[1]
    vm = pl.BlockSpec(memory_space=VMEM)
    hbm = pl.BlockSpec(memory_space=pl.ANY)
    hw = expert_gate.shape[2]
    sw = shared_gate.shape[1]
    nz = nsp // 2
    return pl.pallas_call(
        functools.partial(layer_kernel, nsp, ntp, cap),
        out_shape=jax.ShapeDtypeStruct((tok, width), BF16),
        in_specs=[vm] * 9 + [hbm] * 7,
        out_specs=vm,
        scratch_shapes=[
            DMA((7,)),
            VMEM((tok, ch), F32),
            VMEM((tok, width), BF16),
            VMEM((tok, width), BF16),
            VMEM((nsp, 8, tok), F32),
            VMEM((ntp, ch, width), BF16),
            VMEM((ntp, tok, ch), BF16),
            VMEM((ntp, 8, tok), F32),
            VMEM((ntp, 8, tok), F32),
            DMA((3, 2)), DMA((ntp, 2)),
            DMA((ntp - 1,)), DMA((ntp - 1,)),
            DMA((ntp - 1,)), DMA((ntp - 1,)),
            DMA((nsp - 1,)), DMA((nsp - 1,)),
            VMEM((nsp, ntp, tok, width), BF16),
            VMEM((ntp, width, hw), BF16),
            VMEM((ntp, width, hw), BF16),
            VMEM((ntp, width, sw), BF16),
            VMEM((ntp, width, sw), BF16),
            VMEM((ntp, hw, width), BF16),
            VMEM((ntp, sw, width), BF16),
            VMEM((2, 2, tok, hw), F32),
            VMEM((nsp, ntp, cap, hw), BF16),
            VMEM((ntp, tok, sw), BF16),
            VMEM((nsp, cap, width), BF16),
            VMEM((nsp, cap, width), BF16),
            VMEM((tok, width), F32),
            DMA((1,)),
            DMA((nsp, ntp, 2)),
            DMA((nz - 1, 2)),
            DMA((nz, 2)), DMA((nz, 2)), DMA((nz, 2)),
            DMA((nz, ntp, 2)),
            DMA((nsp, 3, 2)), DMA((nsp, ntp, 2)),
            DMA((3, 2)), DMA((ntp, 2)),
            DMA((nsp,)), DMA((nsp,)),
        ],
        compiler_params=pltpu.CompilerParams(
            collective_id=1, has_side_effects=True, vmem_limit_bytes=60 << 20
        ),
        name="layer",
    )(
        padded, conv_weight, conv_bias[None, :], ln_gain[None, :], ln_bias[None, :], resid, norm_gain[None, :], table, poscol,
        proj_weight.reshape(ntp, ch, width),
        expert_gate[0].reshape(ntp, width, hw),
        expert_up[0].reshape(ntp, width, hw),
        shared_gate.reshape(ntp, width, sw),
        shared_up.reshape(ntp, width, sw),
        expert_down[0].reshape(ntp, hw, width),
        shared_down.reshape(ntp, sw, width),
    )


def chosen(*args):
    tok, width = args[7].shape
    nsp = lax.axis_size("sp")
    ntp = lax.axis_size("tp")
    cap = 2 * tok * args[9].shape[1] // nsp
    fits = 2 * nsp * ntp * tok * width <= 16 << 20
    aligned = tok % 256 == 0 and width % 128 == 0 and cap % 128 == 0
    if ntp == 4 and nsp % 2 == 0 and fits and aligned:
        return fast_shards(*args)
    return shards(*args)


def solution(mesh):
    in_specs = (
        P("sp", "tp"),
        P("sp", "tp"),
        P(None, "tp"),
        P("tp"),
        P("tp"),
        P("tp"),
        P(None, "tp"),
        P("sp", "tp"),
        P("tp"),
        P("sp", None),
        P("sp", None),
        P("sp", None, "tp"),
        P("sp", None, "tp"),
        P("sp", None, "tp"),
        P(None, "tp"),
        P(None, "tp"),
        P(None, "tp"),
    )
    out_specs = P("sp", "tp")
    return jax.shard_map(chosen, mesh=mesh, in_specs=in_specs, out_specs=out_specs, check_vma=False)
```
